1024 devices in a mesh: sp: 16 (over z), dp: 64 (over y, x, core).
Axes of the slice: x: 4, y: 8, z: 16, core: 2. Of those that a mesh axis runs over, the one named last changes fastest.
Arguments:
- queries: bfloat16 [64, 3072, 1024], P('dp', 'sp'), may hold values from -6 to 6
- keys: bfloat16 [64, 3072, 256], P('dp', 'sp'), may hold values from -6 to 6
- values: bfloat16 [64, 3072, 256], P('dp', 'sp'), may hold values from -6 to 6
- query_gain: float32 [64], replicated, may hold values from 0.15 to 7
- key_gain: float32 [64], replicated, may hold values from 0.15 to 7
- out_weight: bfloat16 [1024, 2048], P(None, 'dp'), may hold values from -0.1875 to 0.1875
- out_gain: float32 [2048], replicated, may hold values from 0.1 to 1.9
Outputs:
- output: bfloat16 [64, 3072, 2048], P('dp', 'sp')
The draws below stay inside these ranges and needn't reach their ends.
All inputs are finite; a program needn't handle non-finite values.
Results may differ from the reference program's by a relative error of at most 0.0035.
The reference program's roundings to bfloat16 on the way (of `attn_weights` and `attended`) count: a program that leaves them out, or rounds other values in their place, can miss the bound.
Values may be sent and summed in bfloat16 or wider, within the bound.
A program may use at most 64 MiB of HBM per device.

```python
import jax
import jax.numpy as jnp
from jax import lax

D = 2048
QH = 16
KVH = 4
HEAD = 64
GRID_W = 64
SEQ = 3072
N_DP = 64


def query_key_pair(key):
    base_key = jax.random.fold_in(key, 11)
    key_a, key_b = jax.random.split(base_key, 2)
    key_draw = jax.random.normal(key_a, (N_DP, SEQ, KVH, HEAD), jnp.float32)
    query_draw = jax.random.normal(key_b, (N_DP, SEQ, QH, HEAD), jnp.float32)
    query_draw = jnp.clip(query_draw, -6.0, 6.0).reshape(N_DP, SEQ, QH * HEAD)
    key_draw = jnp.clip(key_draw, -6.0, 6.0).reshape(N_DP, SEQ, KVH * HEAD)
    return (query_draw, key_draw)


def gain_draw(key, salt):
    spread = 1.0 + 0.18 * jnp.clip(jax.random.normal(jax.random.fold_in(key, salt), (HEAD,), jnp.float32), -4.5, 4.5)
    return spread


def draw_queries(key, part):
    return query_key_pair(key)[0].astype(jnp.bfloat16)


def draw_keys(key, part):
    return query_key_pair(key)[1].astype(jnp.bfloat16)


def draw_query_gain(key, part):
    return gain_draw(key, 21)


def draw_key_gain(key, part):
    return gain_draw(key, 22)


def levels(stream_key, dims, cuts, least, largest):
    def one(dim, parts):
        steps = jax.random.uniform(jax.random.fold_in(jax.random.fold_in(stream_key, 6), dim), (parts,), jnp.float32, least / len(cuts), largest / len(cuts))
        return jnp.repeat(jnp.exp(steps), dims[dim] // parts).reshape((-1,) + (1,) * (len(dims) - dim - 1))

    level = one(*cuts[0])
    for cut in cuts[1:]:
        level = level * one(*cut)
    return level


def bell_draw(own_key, extent, scale, most, cuts=(), held_as=jnp.bfloat16):
    factor_of = levels(own_key, extent, cuts, -0.22, 0.18) if cuts else 1.0
    values = jax.random.normal(own_key, extent, jnp.float32) * scale * factor_of
    return jnp.minimum(jnp.maximum(values, -most), most).astype(held_as)


def setup_inputs(seed: int = 0) -> dict:
    streams_of = jax.random.split(jax.random.key(seed), 8)
    return {
        "queries": draw_queries(jax.random.fold_in(streams_of[7], 71), 0),
        "keys": draw_keys(jax.random.fold_in(streams_of[7], 71), 0),
        "values": bell_draw(streams_of[2], (N_DP, SEQ, KVH * HEAD), 1.0, 6.0, ((0, 64), (1, 16))),
        "query_gain": draw_query_gain(jax.random.fold_in(streams_of[7], 71), 0),
        "key_gain": draw_key_gain(jax.random.fold_in(streams_of[7], 71), 0),
        "out_weight": bell_draw(streams_of[5], (QH * HEAD, D), (QH * HEAD) ** -0.5, 0.1875, ((1, 64),)),
        "out_gain": jnp.clip(1.0 + 0.18 * jax.random.normal(streams_of[6], (D,), jnp.float32), 0.1, 1.9),
    }


EPSILON = 1e-06
ROTARY_BASE = 10000.0

def rotate(vectors, positions, width):
    half_width = width // 2
    frequency = ROTARY_BASE ** (-jnp.arange(0, width, 2, dtype=jnp.float32) / width)
    angles = positions.astype(jnp.float32)[:, None] * frequency[None, :]
    cosines = jnp.cos(angles)[:, None, :]
    sine_table = jnp.sin(angles)[:, None, :]
    first_half = vectors[..., :half_width]
    second_half = vectors[..., half_width:]
    return jnp.concatenate([first_half * cosines - second_half * sine_table, second_half * cosines + first_half * sine_table], axis=-1)

def prepare(vectors, gain_vector, grid_row, grid_col):
    vectors = vectors.astype(jnp.float32)
    vectors = vectors * lax.rsqrt(lax.optimization_barrier(jnp.mean(vectors * vectors, axis=-1, keepdims=True)) + EPSILON) * gain_vector
    half_width = HEAD // 2
    turned = jnp.concatenate([rotate(vectors[..., :half_width], grid_row, half_width), rotate(vectors[..., half_width:], grid_col, half_width)], axis=-1)
    return turned.astype(jnp.bfloat16)

def reference(queries, keys, values, query_gain, key_gain, out_weight, out_gain):
    positions = jnp.arange(SEQ, dtype=jnp.int32)
    grid_row = positions // GRID_W
    grid_col = positions % GRID_W
    group_size = QH // KVH
    score_scale = HEAD ** (-0.5)

    def one_sequence(operands):
        query_seq, key_seq, value_seq = operands
        query_rot = prepare(query_seq.reshape(SEQ, QH, HEAD), query_gain, grid_row, grid_col)
        key_rot = prepare(key_seq.reshape(SEQ, KVH, HEAD), key_gain, grid_row, grid_col)
        value_heads = value_seq.reshape(SEQ, KVH, HEAD)

        def one_head(head_index):
            query_head = lax.dynamic_index_in_dim(query_rot, head_index, 1, keepdims=False)
            key_head = lax.dynamic_index_in_dim(key_rot, head_index // group_size, 1, keepdims=False)
            value_head = lax.dynamic_index_in_dim(value_heads, head_index // group_size, 1, keepdims=False)
            scores = jnp.dot(query_head, key_head.T, preferred_element_type=jnp.float32) * score_scale
            row_max = lax.optimization_barrier(jnp.max(scores, axis=-1, keepdims=True))
            exponent = jnp.exp(scores - row_max)
            attn_weights = (exponent / lax.optimization_barrier(jnp.sum(exponent, axis=-1, keepdims=True))).astype(jnp.bfloat16)
            return jnp.dot(attn_weights, value_head, preferred_element_type=jnp.float32).astype(jnp.bfloat16)
        per_head = lax.map(one_head, jnp.arange(QH, dtype=jnp.int32))
        attended = per_head.transpose(1, 0, 2).reshape(SEQ, QH * HEAD)
        projected = jnp.dot(attended, out_weight, preferred_element_type=jnp.float32)
        projected = projected * lax.rsqrt(lax.optimization_barrier(jnp.mean(projected * projected, axis=-1, keepdims=True)) + EPSILON) * out_gain
        return projected.astype(jnp.bfloat16)
    return lax.map(one_sequence, (queries, keys, values))
```

```python
import functools
import math

import jax
import jax.numpy as jnp
import numpy as np
from jax import lax
from jax.experimental import pallas as pl
from jax.experimental.pallas import tpu as pltpu
from jax.sharding import PartitionSpec as P

MESH = pl.DeviceIdType.MESH
F32 = jnp.float32
BF16 = jnp.bfloat16
NZ = 16
NX, NY = 4, 8
TOK = 192
LOG2E = math.log2(math.e)
EPS = 1e-06
MID = 10
SLOTS = 21
NC = 2
LAG = 1
TICKS = 9
WTICKS = 20


def tables():
    freq = (10000.0 ** (-(np.arange(0, 32, 2, dtype=np.float32) / np.float32(32)))).astype(np.float32)
    lane = np.arange(256)
    is_row = lane % 64 < 32
    first = lane % 32 < 16
    sign = np.where(first, -1.0, 1.0)
    by_lane = freq[lane % 16]
    row_angle = (np.arange(48, dtype=np.float32)[:, None] * by_lane[None]).astype(np.float64)
    col_angle = (np.arange(64, dtype=np.float32)[:, None] * by_lane[None]).astype(np.float64)
    row_tab = np.zeros((NZ, 2, 8, 256), np.float32)
    row_tab[:, 0, :3] = np.where(is_row, np.cos(row_angle), 0).reshape(NZ, 3, 256)
    row_tab[:, 1, :3] = np.where(is_row, np.sin(row_angle) * sign, 0).reshape(NZ, 3, 256)
    col_tab = np.stack([np.where(is_row, 0, np.cos(col_angle)), np.where(is_row, 0, np.sin(col_angle) * sign)])
    partner = np.where(first, lane + 16, lane - 16)
    mats = np.zeros((2, 256, 256), np.float32)
    mats[0, partner, lane] = 1
    mats[1] = (lane[:, None] // 64 == lane[None] // 64) / 64.0
    return row_tab, col_tab.astype(np.float32), mats.astype(jnp.bfloat16)


def n_right(z):
    one = lambda c: jnp.where(c, 1, 0).astype(jnp.int32)
    return 6 + one(z >= 2) + one(z >= 4) - one(z >= 9)


def delay(z):
    one = lambda c: jnp.where(c, 1, 0).astype(jnp.int32)
    return 3 - one(z >= 2) - one(z >= 4) - one(z >= 5)


def gain_rows(gain):
    two = jnp.broadcast_to(jnp.concatenate([gain, gain], axis=1), (8, 128))
    lane = lax.broadcasted_iota(jnp.int32, (8, 128), 1)
    swapped = jnp.where(lane % 32 < 16, pltpu.roll(two, 112, 1), pltpu.roll(two, 16, 1))
    wide = lambda a: jnp.concatenate([a, a], axis=1)[0:1]
    return wide(two), wide(swapped)


def rope(x, gain, row_tab, col_tab, mats):
    g, gp = gain
    xf = x.astype(F32)
    sq = xf * xf
    hi = sq.astype(BF16)
    lo = (sq - hi.astype(F32)).astype(BF16)
    mean = jnp.dot(hi, mats[1], preferred_element_type=F32) + jnp.dot(lo, mats[1], preferred_element_type=F32)
    xp = jnp.dot(x, mats[0], preferred_element_type=F32)
    r = lax.rsqrt(mean + EPS)
    parts = []
    for i in range(3):
        rows = slice(64 * i, 64 * i + 64)
        c = (col_tab[0] + row_tab[0, i : i + 1, :]) * g
        s = (col_tab[1] + row_tab[1, i : i + 1, :]) * gp
        parts.append((xf[rows] * c + xp[rows] * s) * r[rows])
    return jnp.concatenate(parts, axis=0)


def kernel(
    q_hbm, k_hbm, v_hbm, w_hbm, qg_ref, kg_ref, og_ref, row_hbm, col_hbm, mats_hbm,
    out_ref,
    qb, kraw, wraw, row_tab, col_tab, mats,
    KB, VB, VT, WB, QX, KX, M, L, MB, E, OT, ATT, PROJ,
    in_sem, ks_sem, kr_sem, vs_sem, vr_sem, wx_ss, wx_rs, wy_ss, wy_rs, wd_ss, wd_rs,
):
    z = lax.axis_index("sp")
    d = lax.axis_index("dp")
    core = d % 2
    x = (d // 2) % NX
    y = d // (2 * NX)
    up, down = (z + 1) % NZ, (z + NZ - 1) % NZ
    at = lambda xx, yy, cc: (z, (yy * NX + xx) * 2 + cc)
    nR = n_right(z)
    nL = (NZ - 1) - nR
    low = MID - nR

    loads = [
        pltpu.make_async_copy(k_hbm.at[0], kraw, in_sem.at[0]),
        pltpu.make_async_copy(row_hbm.at[z], row_tab, in_sem.at[1]),
        pltpu.make_async_copy(col_hbm, col_tab, in_sem.at[2]),
        pltpu.make_async_copy(mats_hbm, mats, in_sem.at[3]),
        pltpu.make_async_copy(v_hbm.at[0], VB.at[MID], in_sem.at[4]),
        pltpu.make_async_copy(w_hbm, wraw, in_sem.at[5]),
        pltpu.make_async_copy(q_hbm.at[0], qb, in_sem.at[6]),
    ]
    for c in loads:
        c.start()

    barrier = pltpu.get_barrier_semaphore()
    sib = at(x, y, 1 - core)
    partners = [
        (up, d), (down, d),
        at((x + 1) % NX, y, core), at((x + 2) % NX, y, core), at((x + 3) % NX, y, core),
        at(x, (y + 1) % NY, core), at(x, (y + NY - 1) % NY, core), sib,
    ]
    for p in partners:
        pl.semaphore_signal(barrier, inc=1, device_id=p, device_id_type=MESH)

    for c in loads[:4]:
        c.wait()
    kg = gain_rows(kg_ref[...])
    KB[MID] = rope(kraw[...], kg, row_tab, col_tab, mats).astype(BF16)
    loads[4].wait()
    loads[5].wait()
    eye = (lax.broadcasted_iota(jnp.int32, (32, 32), 0) == lax.broadcasted_iota(jnp.int32, (32, 32), 1)).astype(BF16)
    own_w = lax.dot_general(eye, wraw[...], (((1,), (1,)), ((), ())), preferred_element_type=F32)
    WB[d] = own_w.astype(BF16)
    pl.semaphore_wait(barrier, len(partners))

    def kv(buf, ss, rs, b, sg, c):
        rows = pl.ds(c * (TOK // NC), TOK // NC)
        return pltpu.make_async_remote_copy(
            src_ref=buf.at[b, rows], dst_ref=buf.at[b + sg, rows], send_sem=ss.at[b + sg, c],
            recv_sem=rs.at[b + sg, c], device_id=((z - sg + NZ) % NZ, d), device_id_type=MESH,
        )

    def own(buf, ss, rs):
        for c in range(NC):
            for sg in (-1, 1):
                kv(buf, ss, rs, MID, sg, c).start()

    def arrive(buf, ss, rs, sg, k):
        b = MID + sg * k
        there = (z - sg + NZ) % NZ
        most = jnp.where(sg < 0, n_right(there), (NZ - 1) - n_right(there))
        for c in range(NC):
            kv(buf, ss, rs, b - sg, sg, c).wait_recv()

            @pl.when(k + 1 <= most)
            def _():
                kv(buf, ss, rs, b, sg, c).start()

    def sent(buf, ss, rs, sg, k):
        there = (z - sg + NZ) % NZ
        most = jnp.where(sg < 0, n_right(there), (NZ - 1) - n_right(there))

        @pl.when(k + 1 <= most)
        def _():
            for c in range(NC):
                kv(buf, ss, rs, MID + sg * k, sg, c).wait_send()

    own(KB, ks_sem, kr_sem)
    own(VB, vs_sem, vr_sem)

    def wx(j):
        return pltpu.make_async_remote_copy(
            src_ref=WB.at[d], dst_ref=WB.at[d], send_sem=wx_ss.at[j], recv_sem=wx_rs.at[j],
            device_id=at((x + NX - j) % NX, y, core), device_id_type=MESH,
        )

    def wblock(j, s):
        return (((y + NY - s) % NY) * NX + (x + j) % NX) * 2 + core

    def wy(j, s, sg):
        blk = wblock(j, NY - sg * s if not isinstance(s, int) else (-sg * s) % NY)
        return pltpu.make_async_remote_copy(
            src_ref=WB.at[blk], dst_ref=WB.at[blk], send_sem=wy_ss.at[(sg + 1) // 2, j, s + 1],
            recv_sem=wy_rs.at[(sg + 1) // 2, j, s + 1],
            device_id=at(x, (y - sg + NY) % NY, core), device_id_type=MESH,
        )

    def wd(blk):
        return pltpu.make_async_remote_copy(
            src_ref=WB.at[blk], dst_ref=WB.at[blk], send_sem=wd_ss.at[blk // 2], recv_sem=wd_rs.at[blk // 2],
            device_id=sib, device_id_type=MESH,
        )

    for j in (1, 2, 3):
        wx(j).start()
    wd(d).start()

    def w_side(j, s, sg, upto):
        most = upto(j, sg)
        blk = wblock(j, NY - sg * s)

        @pl.when(s <= most)
        def _():
            wy(j, s - 1, sg).wait_recv()
            wd(blk).start()

        @pl.when(s + 1 <= most)
        def _():
            wy(j, s, sg).start()

    def upto(j, sg):
        even = jnp.where(j % 2 == 0, 1, 0)
        return jnp.where(sg < 0, 3 + even, 4 - even)

    def w_tick(i):
        s, j = i // 4, i % 4

        @pl.when(s == 0)
        def _():
            @pl.when(j > 0)
            def _():
                wx(j).wait_recv()
                wd(wblock(j, 0)).start()

            wy(j, s, -1).start()
            wy(j, s, 1).start()

        @pl.when(s > 0)
        def _():
            w_side(j, s, -1, upto)
            w_side(j, s, 1, upto)

    loads[6].wait()
    qg = gain_rows(qg_ref[...])
    lane = lax.broadcasted_iota(jnp.int32, (64, 128), 1)

    def put(t, half, val):
        hi = val.astype(BF16)
        rest = val - hi.astype(F32)
        mid = rest.astype(BF16)
        lo = (rest - mid.astype(F32)).astype(BF16)
        cols = slice(128 * half, 128 * half + 128)
        QX[t, 0:64, cols] = hi
        QX[t, 64:128, cols] = mid
        QX[t, 128:192, cols] = lo
        QX[t, 192:256, cols] = jnp.zeros((64, 128), BF16)

    for g in range(4):
        qr = rope(qb[:, 256 * g : 256 * g + 256], qg, row_tab, col_tab, mats)
        qr = qr.astype(BF16).astype(F32) * (0.125 * LOG2E)
        a = jnp.transpose(qr[0:128])
        b = jnp.transpose(jnp.concatenate([qr[128:192], jnp.zeros((64, 256), F32)], axis=0))
        for r in range(4):
            put(3 * g + r // 2, r % 2, a[64 * r : 64 * r + 64])
        for h in range(2):
            b0, b1 = b[128 * h : 128 * h + 64], pltpu.roll(b[128 * h + 64 : 128 * h + 128], 64, 1)
            put(3 * g + 2, h, jnp.where(lane < 64, b0, b1))
    M[...] = jnp.full_like(M, -1e30)
    L[...] = jnp.zeros_like(L)
    OT[...] = jnp.zeros_like(OT)
    lane2 = lax.broadcasted_iota(jnp.int32, (TOK, 128), 1)

    def pass1(b):
        for pr in range(2):
            v = KB[b, :, 128 * pr : 128 * pr + 128].astype(F32)
            rt = pltpu.roll(v, 64, 1)
            for o in range(2):
                dup = jnp.where(lane2 < 64, v, rt) if o == 0 else jnp.where(lane2 < 64, rt, v)
                dup = dup.astype(BF16)
                KX[2 * pr + o, :, 0:128] = dup
                KX[2 * pr + o, :, 128:256] = dup
        i = b - low
        for t in range(12):
            s = jnp.dot(KX[t // 3], QX[t], preferred_element_type=F32).reshape(TOK // 8, 8, 256)
            old = M[t]
            new = jnp.maximum(old, jnp.max(s, axis=0))
            e = jnp.exp2(s - new[None])
            L[t] = L[t] * jnp.exp2(old - new) + jnp.sum(e, axis=0)
            M[t] = new
            MB[i, t] = new
            E[i, t] = e.reshape(TOK, 256)

    def turn_v(b):
        v = VB[b].astype(F32)
        i = b - low
        VT[i, :, 0:128] = jnp.transpose(v[0:128]).astype(BF16)
        VT[i, :, 128:256] = jnp.transpose(jnp.concatenate([v[128:192], jnp.zeros((64, 256), F32)], axis=0)).astype(BF16)

    def pass2(i):
        for t in range(12):
            g = t // 3
            f = jnp.exp2(MB[i, t] - M[t])
            p = (E[i, t].reshape(TOK // 8, 8, 256) * f[None]).reshape(TOK, 256).astype(BF16)
            OT[t] += jnp.dot(VT[i, 64 * g : 64 * g + 64, 0:TOK], p, preferred_element_type=F32)

    pass1(MID)
    turn_v(MID)
    late = delay(z)

    def tick(t, carry):
        def side(j, c2):
            sg = 1 - 2 * j
            k_plain = t + 1
            k_late = t + 1 - late
            k = jnp.where((sg > 0) | (k_plain <= z), k_plain, k_late)
            ok = jnp.where(sg > 0, k <= nL, (k <= nR) & ((k_plain <= z) | (k_late > z)))

            @pl.when(ok)
            def _():
                arrive(KB, ks_sem, kr_sem, sg, k)

                @pl.when(k > LAG)
                def _():
                    arrive(VB, vs_sem, vr_sem, sg, k - LAG)
                    turn_v(MID + sg * (k - LAG))

                pass1(MID + sg * k)

            @pl.when(2 * t + j < WTICKS)
            def _():
                w_tick(2 * t + j)

            return c2

        return lax.fori_loop(0, 2, side, carry)

    lax.fori_loop(0, TICKS, tick, 0)

    def w_more(i, c):
        w_tick(i)
        return c

    lax.fori_loop(2 * TICKS, WTICKS, w_more, 0)

    m = M[...]
    top = jnp.max(m, axis=1, keepdims=True)
    total = jnp.sum(L[...] * jnp.exp2(m - top), axis=1, keepdims=True)
    M[...] = jnp.broadcast_to(top + jnp.log(total) * LOG2E, M.shape)

    for sg, n in ((1, nL), (-1, nR)):
        for back in range(LAG):
            k = n - LAG + 1 + back
            arrive(VB, vs_sem, vr_sem, sg, k)
            turn_v(MID + sg * k)

    def p2(i, c):
        pass2(i)
        return c

    lax.fori_loop(0, NZ, p2, 0)

    for g in range(4):
        for p in range(2):
            a = jnp.concatenate([OT[3 * g + p, :, 0:128], OT[3 * g + p, :, 128:256]], axis=0)
            ATT[0:128, 256 * g + 128 * p : 256 * g + 128 * p + 128] = jnp.transpose(a).astype(BF16)
            b = OT[3 * g + 2, :, 128 * p : 128 * p + 128]
            b = jnp.transpose(jnp.concatenate([b, b], axis=0))
            ATT[128:192, 256 * g + 128 * p : 256 * g + 128 * p + 128] = jnp.where(lane < 64, b[0:64], b[64:128]).astype(BF16)

    def w_in(i, c):
        wd(2 * i + 1 - core).wait_recv()
        return c

    lax.fori_loop(0, NX * NY, w_in, 0)

    def project(n, ss):
        w = WB[pl.ds(8 * n, 8)].reshape(256, 1024)
        pr = lax.dot_general(ATT[...], w, (((1,), (1,)), ((), ())), preferred_element_type=F32)
        PROJ[n] = pr
        sq = pr * pr
        return ss + sq[:, 0:128] + sq[:, 128:256]

    ss = lax.fori_loop(0, 8, project, jnp.zeros((TOK, 128), F32))
    r = lax.rsqrt(jnp.sum(ss, axis=1, keepdims=True) / 2048.0 + EPS)
    for n in range(8):
        cols = slice(256 * n, 256 * n + 256)
        out_ref[0, :, cols] = (PROJ[n] * r * og_ref[:, cols]).astype(BF16)

    def out_kv(k, c):
        for sg in (-1, 1):
            sent(KB, ks_sem, kr_sem, sg, k)
            sent(VB, vs_sem, vr_sem, sg, k)
        return c

    lax.fori_loop(0, 10, out_kv, 0)
    for j in (1, 2, 3):
        wx(j).wait_send()

    def out_w(i, c):
        s, j = i // 4, i % 4
        for sg in (-1, 1):

            @pl.when(s + 1 <= upto(j, sg))
            def _():
                wy(j, s, sg).wait_send()

        return c

    lax.fori_loop(0, 16, out_w, 0)

    def out_d(i, c):
        wd(2 * i + core).wait_send()
        return c

    lax.fori_loop(0, NX * NY, out_d, 0)


def per_device(queries, keys, values, query_gain, key_gain, out_weight, out_gain):
    row_tab, col_tab, mats = tables()
    hbm = pl.BlockSpec(memory_space=pl.ANY)
    vmem = pl.BlockSpec(memory_space=pltpu.VMEM)
    dma = pltpu.SemaphoreType.DMA
    return pl.pallas_call(
        kernel,
        out_shape=jax.ShapeDtypeStruct((1, TOK, 2048), BF16),
        in_specs=[hbm, hbm, hbm, hbm, vmem, vmem, vmem, hbm, hbm, hbm],
        out_specs=vmem,
        scratch_shapes=[
            pltpu.VMEM((TOK, 1024), BF16), pltpu.VMEM((TOK, 256), BF16), pltpu.VMEM((1024, 32), BF16),
            pltpu.VMEM((2, 8, 256), F32), pltpu.VMEM((2, 64, 256), F32), pltpu.VMEM((2, 256, 256), BF16),
            pltpu.VMEM((SLOTS, TOK, 256), BF16), pltpu.VMEM((SLOTS, TOK, 256), BF16), pltpu.VMEM((NZ, 256, 256), BF16),
            pltpu.VMEM((64, 32, 1024), BF16), pltpu.VMEM((12, 256, 256), BF16), pltpu.VMEM((4, TOK, 256), BF16),
            pltpu.VMEM((12, 8, 256), F32), pltpu.VMEM((12, 8, 256), F32), pltpu.VMEM((NZ, 12, 8, 256), F32),
            pltpu.VMEM((NZ, 12, TOK, 256), F32), pltpu.VMEM((12, 64, 256), F32), pltpu.VMEM((TOK, 1024), BF16),
            pltpu.VMEM((8, TOK, 256), F32),
            dma((7,)), dma((SLOTS, NC)), dma((SLOTS, NC)), dma((SLOTS, NC)), dma((SLOTS, NC)),
            dma((4,)), dma((4,)), dma((2, 4, 5)), dma((2, 4, 5)), dma((32,)), dma((32,)),
        ],
        compiler_params=pltpu.CompilerParams(
            collective_id=0, has_side_effects=True, vmem_limit_bytes=67043328
        ),
        name="attend",
    )(
        queries, keys, values, out_weight, query_gain[None], key_gain[None], out_gain[None],
        jnp.asarray(row_tab), jnp.asarray(col_tab), jnp.asarray(mats),
    )


def solution(mesh):
    return jax.shard_map(
        per_device,
        mesh=mesh,
        in_specs=(
            P("dp", "sp", None),
            P("dp", "sp", None),
            P("dp", "sp", None),
            P(),
            P(),
            P(None, "dp"),
            P(),
        ),
        out_specs=P("dp", "sp", None),
        check_vma=False,
    )
```

```python
import functools
import math

import jax
import jax.numpy as jnp
import numpy as np
from jax import lax
from jax.experimental import pallas as pl
from jax.experimental.pallas import tpu as pltpu
from jax.sharding import PartitionSpec as P

MESH = pl.DeviceIdType.MESH
F32 = jnp.float32
BF16 = jnp.bfloat16
NZ = 16
NX, NY = 4, 8
TOK = 192
LOG2E = math.log2(math.e)
EPS = 1e-06
MID = 10
SLOTS = 21
NC = 2
WTICKS = 20
N_RIGHT = (7, 7, 7, 7, 7, 7, 7, 7, 7, 7, 7, 7, 7, 7, 7, 7)
ORDER = (
    (328470619, 293635227, 170919067, 293635227, 293635227, 696288411, 176424091, 293635227, 621024411, 621024411, 621024411, 621024411, 621024411, 621024411, 621024411, 696288411),
    (327320203, 192190165, 290326058, 170930389, 170930389, 170930386, 170930389, 170930389, 696288922, 696288922, 696288922, 696288922, 696288922, 696288922, 696288915, 621024467),
    (327320203, 696289001, 192190185, 290326058, 290326058, 290326058, 290326058, 170930410, 696288922, 696288922, 696288922, 696288922, 696288922, 696288922, 696288915, 621024467),
    (327323731, 696288922, 290308137, 410293993, 174702913, 174702913, 290326337, 170930410, 696288922, 696288922, 696288922, 696288922, 696288922, 696288922, 696288915, 621024467),
    (327323731, 170930386, 172867625, 409637984, 547624681, 172898824, 290326337, 170930410, 696288922, 696288922, 696288922, 696288922, 696288922, 696288922, 696288915, 621024467),
    (327323731, 290326037, 174702920, 409555552, 51684051, 696289001, 290326337, 170930410, 696288922, 696288922, 696288922, 696288922, 696288922, 696288922, 696288915, 621024467),
    (694325913, 290326057, 40487432, 409637984, 409637980, 547624147, 691024105, 290326338, 170930330, 696288922, 696288922, 696288922, 696288922, 696288922, 696288915, 621024467),
    (1055471384, 376029505, 860705537, 508469856, 510301280, 1047831195, 1047828122, 1047828201, 1047828181, 1047828122, 1047828122, 1047828122, 1047828122, 1047828122, 1047828115, 930387155),
    (1056698302, 937393663, 937394167, 1056701943, 1056931319, 1071611379, 937393651, 937393651, 937393651, 937393651, 937393651, 937393651, 937393651, 937393651, 937393651, 1056698299),
    (920350135, 920350199, 920350647, 920350654, 920350654, 920350654, 920350711, 920350711, 920350711, 920350711, 920350711, 920350711, 920350711, 920350711, 920350711, 920350654),
)


def tables():
    freq = (10000.0 ** (-(np.arange(0, 32, 2, dtype=np.float32) / np.float32(32)))).astype(np.float32)
    lane = np.arange(256)
    is_row = lane % 64 < 32
    first = lane % 32 < 16
    sign = np.where(first, -1.0, 1.0)
    by_lane = freq[lane % 16]
    row_angle = (np.arange(48, dtype=np.float32)[:, None] * by_lane[None]).astype(np.float64)
    col_angle = (np.arange(64, dtype=np.float32)[:, None] * by_lane[None]).astype(np.float64)
    row_tab = np.zeros((NZ, 2, 8, 256), np.float32)
    row_tab[:, 0, :3] = np.where(is_row, np.cos(row_angle), 0).reshape(NZ, 3, 256)
    row_tab[:, 1, :3] = np.where(is_row, np.sin(row_angle) * sign, 0).reshape(NZ, 3, 256)
    col_tab = np.stack([np.where(is_row, 0, np.cos(col_angle)), np.where(is_row, 0, np.sin(col_angle) * sign)])
    partner = np.where(first, lane + 16, lane - 16)
    mats = np.zeros((2, 256, 256), np.float32)
    mats[0, partner, lane] = 1
    mats[1] = (lane[:, None] // 64 == lane[None] // 64) / 64.0
    return row_tab, col_tab.astype(np.float32), mats.astype(jnp.bfloat16)


def pick(values, z):
    out = jnp.int32(values[0])
    for i, v in enumerate(values[1:], 1):
        if v != values[0]:
            out = jnp.where(z == i, jnp.int32(v), out)
    return out


def gain_rows(gain):
    two = jnp.broadcast_to(jnp.concatenate([gain, gain], axis=1), (8, 128))
    lane = lax.broadcasted_iota(jnp.int32, (8, 128), 1)
    swapped = jnp.where(lane % 32 < 16, pltpu.roll(two, 112, 1), pltpu.roll(two, 16, 1))
    wide = lambda a: jnp.concatenate([a, a], axis=1)[0:1]
    return wide(two), wide(swapped)


def rope(x, gain, row_tab, col_tab, mats):
    g, gp = gain
    xf = x.astype(F32)
    sq = xf * xf
    hi = sq.astype(BF16)
    lo = (sq - hi.astype(F32)).astype(BF16)
    mean = jnp.dot(hi, mats[1], preferred_element_type=F32) + jnp.dot(lo, mats[1], preferred_element_type=F32)
    xp = jnp.dot(x, mats[0], preferred_element_type=F32)
    r = lax.rsqrt(mean + EPS)
    parts = []
    for i in range(3):
        rows = slice(64 * i, 64 * i + 64)
        c = (col_tab[0] + row_tab[0, i : i + 1, :]) * g
        s = (col_tab[1] + row_tab[1, i : i + 1, :]) * gp
        parts.append((xf[rows] * c + xp[rows] * s) * r[rows])
    return jnp.concatenate(parts, axis=0)


def kernel(
    q_hbm, k_hbm, v_hbm, w_hbm, qg_ref, kg_ref, og_ref, row_hbm, col_hbm, mats_hbm,
    out_ref,
    qb, kraw, row_tab, col_tab, mats,
    KV, VT, WB, QX, KX, M, L, MB, E, OT, ATT, PROJ,
    in_sem, s_sem, r_sem, wx_ss, wx_rs, wy_ss, wy_rs, wd_ss, wd_rs, late_sem,
):
    z = lax.axis_index("sp")
    d = lax.axis_index("dp")
    core = d & 1
    x = (d >> 1) & (NX - 1)
    y = d >> 3
    up, down = (z + 1) & (NZ - 1), (z - 1) & (NZ - 1)
    at = lambda xx, yy, cc: (z, (yy * NX + xx) * 2 + cc)
    nR = pick(N_RIGHT, z)
    nL = (NZ - 1) - nR
    low = MID - nR

    loads = [
        pltpu.make_async_copy(k_hbm.at[0], kraw, in_sem.at[0]),
        pltpu.make_async_copy(row_hbm.at[z], row_tab, in_sem.at[1]),
        pltpu.make_async_copy(col_hbm, col_tab, in_sem.at[2]),
        pltpu.make_async_copy(mats_hbm, mats, in_sem.at[3]),
        pltpu.make_async_copy(v_hbm.at[0], KV.at[MID + SLOTS], in_sem.at[4]),
        pltpu.make_async_copy(w_hbm, WB.at[d], in_sem.at[5]),
        pltpu.make_async_copy(q_hbm.at[0], qb, in_sem.at[6]),
    ]
    for c in loads:
        c.start()

    barrier = pltpu.get_barrier_semaphore()
    sib = at(x, y, 1 - core)
    partners = [
        (down, d),
        at((x + 1) & (NX - 1), y, core), at((x + 2) & (NX - 1), y, core), at((x + 3) & (NX - 1), y, core),
        at(x, (y + 1) & (NY - 1), core), at(x, (y - 1) & (NY - 1), core), sib,
    ]
    for p in partners:
        pl.semaphore_signal(barrier, inc=1, device_id=p, device_id_type=MESH)

    @pl.when(z != NZ - 1)
    def _():
        pl.semaphore_signal(barrier, inc=1, device_id=(up, d), device_id_type=MESH)

    for c in loads[:4]:
        c.wait()
    kg = gain_rows(kg_ref[...])
    KV[MID] = rope(kraw[...], kg, row_tab, col_tab, mats).astype(BF16)
    loads[4].wait()
    loads[5].wait()
    pl.semaphore_wait(barrier, len(partners) + jnp.where(z == 0, 0, 1))

    @pl.when(z == NZ - 1)
    def _():
        pl.semaphore_signal(late_sem, inc=1, device_id=(0, d), device_id_type=MESH)

    there = lambda sg: jnp.where(sg < 0, up, down)

    def kv(b, sg, c):
        rows = pl.ds(c * (TOK // NC), TOK // NC)
        return pltpu.make_async_remote_copy(
            src_ref=KV.at[b, rows], dst_ref=KV.at[b + sg, rows], send_sem=s_sem.at[b + sg, c],
            recv_sem=r_sem.at[b + sg, c], device_id=(there(sg), d), device_id_type=MESH,
        )

    def own(b, sg):
        for c in range(NC):
            kv(b, sg, c).start()

    own(MID, -1)

    @pl.when(z == 0)
    def _():
        own(MID + SLOTS, -1)

    @pl.when(z != 0)
    def _():
        own(MID, 1)

    def wx(j):
        return pltpu.make_async_remote_copy(
            src_ref=WB.at[d], dst_ref=WB.at[d], send_sem=wx_ss.at[j], recv_sem=wx_rs.at[j],
            device_id=at((x - j) & (NX - 1), y, core), device_id_type=MESH,
        )

    def wblock(j, s):
        return (((y - s) & (NY - 1)) * NX + ((x + j) & (NX - 1))) * 2 + core

    def wy(j, s, sg):
        blk = wblock(j, -sg * s)
        return pltpu.make_async_remote_copy(
            src_ref=WB.at[blk], dst_ref=WB.at[blk], send_sem=wy_ss.at[(sg + 1) >> 1, j, s + 1],
            recv_sem=wy_rs.at[(sg + 1) >> 1, j, s + 1],
            device_id=at(x, (y - sg) & (NY - 1), core), device_id_type=MESH,
        )

    def wd(blk):
        return pltpu.make_async_remote_copy(
            src_ref=WB.at[blk], dst_ref=WB.at[blk], send_sem=wd_ss.at[blk >> 1], recv_sem=wd_rs.at[blk >> 1],
            device_id=sib, device_id_type=MESH,
        )

    for j in (1, 2, 3):
        wx(j).start()
    wd(d).start()

    def w_side(j, s, sg, upto):
        most = upto(j, sg)
        blk = wblock(j, -sg * s)

        @pl.when(s <= most)
        def _():
            wy(j, s - 1, sg).wait_recv()
            wd(blk).start()

        @pl.when(s + 1 <= most)
        def _():
            wy(j, s, sg).start()

    def upto(j, sg):
        even = 1 - (j & 1)
        return jnp.where(sg < 0, 3 + even, 4 - even)

    def w_tick(i):
        s, j = i >> 2, i & 3

        @pl.when(s == 0)
        def _():
            @pl.when(j > 0)
            def _():
                wx(j).wait_recv()
                wd(wblock(j, 0)).start()

            wy(j, s, -1).start()
            wy(j, s, 1).start()

        @pl.when(s > 0)
        def _():
            w_side(j, s, -1, upto)
            w_side(j, s, 1, upto)

    loads[6].wait()
    qg = gain_rows(qg_ref[...])
    lane = lax.broadcasted_iota(jnp.int32, (64, 128), 1)

    def put(t, half, val):
        hi = val.astype(BF16)
        rest = val - hi.astype(F32)
        mid = rest.astype(BF16)
        lo = (rest - mid.astype(F32)).astype(BF16)
        cols = slice(128 * half, 128 * half + 128)
        QX[t, 0:64, cols] = hi
        QX[t, 64:128, cols] = mid
        QX[t, 128:192, cols] = lo
        QX[t, 192:256, cols] = jnp.zeros((64, 128), BF16)

    for g in range(4):
        qr = rope(qb[:, 256 * g : 256 * g + 256], qg, row_tab, col_tab, mats)
        qr = qr.astype(BF16).astype(F32) * (0.125 * LOG2E)
        a = jnp.transpose(qr[0:128])
        b = jnp.transpose(jnp.concatenate([qr[128:192], jnp.zeros((64, 256), F32)], axis=0))
        for r in range(4):
            put(3 * g + r // 2, r % 2, a[64 * r : 64 * r + 64])
        for h in range(2):
            b0, b1 = b[128 * h : 128 * h + 64], pltpu.roll(b[128 * h + 64 : 128 * h + 128], 64, 1)
            put(3 * g + 2, h, jnp.where(lane < 64, b0, b1))
    M[...] = jnp.full_like(M, -1e30)
    L[...] = jnp.zeros_like(L)
    OT[...] = jnp.zeros_like(OT)
    lane2 = lax.broadcasted_iota(jnp.int32, (TOK, 128), 1)

    def pass1(b):
        for pr in range(2):
            v = KV[b, :, 128 * pr : 128 * pr + 128].astype(F32)
            rt = pltpu.roll(v, 64, 1)
            for o in range(2):
                dup = jnp.where(lane2 < 64, v, rt) if o == 0 else jnp.where(lane2 < 64, rt, v)
                dup = dup.astype(BF16)
                KX[2 * pr + o, :, 0:128] = dup
                KX[2 * pr + o, :, 128:256] = dup
        i = b - low
        for t in range(12):
            s = jnp.dot(KX[t // 3], QX[t], preferred_element_type=F32).reshape(TOK // 8, 8, 256)
            old = M[t]
            new = jnp.maximum(old, jnp.max(s, axis=0))
            e = jnp.exp2(s - new[None])
            L[t] = L[t] * jnp.exp2(old - new) + jnp.sum(e, axis=0)
            M[t] = new
            MB[i, t] = new
            E[i, t] = e.reshape(TOK, 256)

    def turn_v(b):
        v = KV[b + SLOTS].astype(F32)
        i = b - low
        VT[i, :, 0:128] = jnp.transpose(v[0:128]).astype(BF16)
        VT[i, :, 128:256] = jnp.transpose(jnp.concatenate([v[128:192], jnp.zeros((64, 256), F32)], axis=0)).astype(BF16)

    def pass2(i):
        turn_v(i + low)
        for t in range(12):
            g = t // 3
            f = jnp.exp2(MB[i, t] - M[t])
            p = (E[i, t].reshape(TOK // 8, 8, 256) * f[None]).reshape(TOK, 256).astype(BF16)
            OT[t] += jnp.dot(VT[i, 64 * g : 64 * g + 64, 0:TOK], p, preferred_element_type=F32)

    pass1(MID)

    @pl.when(z == 0)
    def _():
        pl.semaphore_wait(late_sem, 1)
        own(MID, 1)

    def finish():
        m = M[...]
        top = jnp.max(m, axis=1, keepdims=True)
        total = jnp.sum(L[...] * jnp.exp2(m - top), axis=1, keepdims=True)
        M[...] = jnp.broadcast_to(top + jnp.log(total) * LOG2E, M.shape)
        pass2(MID - low)

    shift = NC.bit_length() - 1
    right_up, left_down = pick(N_RIGHT[1:] + N_RIGHT[:1], z), (NZ - 1) - pick(N_RIGHT[-1:] + N_RIGHT[:-1], z)

    def step(_, carry):
        word, copies, blocks, done = carry
        digit = word & 7
        side = digit & 1
        sg = 2 * side - 1
        is_copy = digit < 4
        c_at, b_at = 6 * (digit & 3), 4 * (digit & 3)

        @pl.when(is_copy)
        def _():
            n = (copies >> c_at) & 63
            v = digit >> 1
            k = (n >> shift) + 1 - v
            c = n & (NC - 1)
            b = MID + sg * k + SLOTS * v

            @pl.when(k > 0)
            def _():
                kv(b - sg, sg, c).wait_recv()

            @pl.when(k < jnp.where(side == 0, right_up, left_down))
            def _():
                kv(b, sg, c).start()

        n = (blocks >> b_at) & 15
        b = MID + sg * (n + 1)
        is_scores = (digit == 4) | (digit == 5)

        @pl.when(is_scores)
        def _():
            pass1(b)

            def w(j, c):
                w_tick(j)
                return c

            lax.fori_loop((3 * done) >> 1, jnp.minimum((3 * done + 3) >> 1, WTICKS), w, 0)

            @pl.when(done == NZ - 2)
            def _():
                finish()

        @pl.when((digit >= 6) & (n < jnp.where(side == 0, nR, nL)))
        def _():
            pass2(b - low)

        one = jnp.int32(1)
        return (
            word >> 3,
            copies + jnp.where(is_copy, one << c_at, 0),
            blocks + jnp.where(is_copy, 0, one << b_at),
            done + jnp.where(is_scores, 1, 0),
        )

    def ten(_, carry):
        words, counts = carry
        out = lax.fori_loop(0, 10, step, (words[0], *counts))
        return words[1:] + words[:1], out[1:]

    zero = jnp.int32(0)
    counts = (jnp.where(z == 0, jnp.int32(NC << 12), 0), zero, zero)
    lax.fori_loop(0, len(ORDER), ten, (tuple(pick(w, z) for w in ORDER), counts))

    for g in range(4):
        for p in range(2):
            a = jnp.concatenate([OT[3 * g + p, :, 0:128], OT[3 * g + p, :, 128:256]], axis=0)
            ATT[0:128, 256 * g + 128 * p : 256 * g + 128 * p + 128] = jnp.transpose(a).astype(BF16)
            b = OT[3 * g + 2, :, 128 * p : 128 * p + 128]
            b = jnp.transpose(jnp.concatenate([b, b], axis=0))
            ATT[128:192, 256 * g + 128 * p : 256 * g + 128 * p + 128] = jnp.where(lane < 64, b[0:64], b[64:128]).astype(BF16)

    def w_in(i, c):
        wd(2 * i + 1 - core).wait_recv()
        return c

    lax.fori_loop(0, NX * NY, w_in, 0)

    def project(n, ss):
        w = WB[pl.ds(8 * n, 8)].reshape(256, 1024)
        pr = lax.dot_general(ATT[...], w, (((1,), (1,)), ((), ())), preferred_element_type=F32)
        PROJ[n] = pr
        sq = pr * pr
        return ss + sq[:, 0:128] + sq[:, 128:256]

    ss = lax.fori_loop(0, 8, project, jnp.zeros((TOK, 128), F32))
    r = lax.rsqrt(jnp.sum(ss, axis=1, keepdims=True) / 2048.0 + EPS)
    for n in range(8):
        cols = slice(256 * n, 256 * n + 256)
        out_ref[0, :, cols] = (PROJ[n] * r * og_ref[:, cols]).astype(BF16)

    for sg, most in ((-1, right_up), (1, left_down)):

        def gone(k, carry):
            for c in range(NC):
                kv(MID + sg * k, sg, c).wait_send()
                kv(MID + SLOTS + sg * k, sg, c).wait_send()
            return carry

        lax.fori_loop(0, most, gone, 0)

    for j in (1, 2, 3):
        wx(j).wait_send()

    def out_w(i, c):
        s, j = i >> 2, i & 3
        for sg in (-1, 1):

            @pl.when(s + 1 <= upto(j, sg))
            def _():
                wy(j, s, sg).wait_send()

        return c

    lax.fori_loop(0, 16, out_w, 0)

    def out_d(i, c):
        wd(2 * i + core).wait_send()
        return c

    lax.fori_loop(0, NX * NY, out_d, 0)


def per_device(queries, keys, values, query_gain, key_gain, out_weight, out_gain):
    row_tab, col_tab, mats = tables()
    hbm = pl.BlockSpec(memory_space=pl.ANY)
    vmem = pl.BlockSpec(memory_space=pltpu.VMEM)
    dma = pltpu.SemaphoreType.DMA
    return pl.pallas_call(
        kernel,
        out_shape=jax.ShapeDtypeStruct((1, TOK, 2048), BF16),
        in_specs=[hbm, hbm, hbm, hbm, vmem, vmem, vmem, hbm, hbm, hbm],
        out_specs=vmem,
        scratch_shapes=[
            pltpu.VMEM((TOK, 1024), BF16), pltpu.VMEM((TOK, 256), BF16),
            pltpu.VMEM((2, 8, 256), F32), pltpu.VMEM((2, 64, 256), F32), pltpu.VMEM((2, 256, 256), BF16),
            pltpu.VMEM((2 * SLOTS, TOK, 256), BF16), pltpu.VMEM((NZ, 256, 256), BF16),
            pltpu.VMEM((64, 32, 1024), BF16), pltpu.VMEM((12, 256, 256), BF16), pltpu.VMEM((4, TOK, 256), BF16),
            pltpu.VMEM((12, 8, 256), F32), pltpu.VMEM((12, 8, 256), F32), pltpu.VMEM((NZ, 12, 8, 256), F32),
            pltpu.VMEM((NZ, 12, TOK, 256), F32), pltpu.VMEM((12, 64, 256), F32), pltpu.VMEM((TOK, 1024), BF16),
            pltpu.VMEM((8, TOK, 256), F32),
            dma((7,)), dma((2 * SLOTS, NC)), dma((2 * SLOTS, NC)),
            dma((4,)), dma((4,)), dma((2, 4, 5)), dma((2, 4, 5)), dma((32,)), dma((32,)), pltpu.SemaphoreType.REGULAR,
        ],
        compiler_params=pltpu.CompilerParams(
            collective_id=0, has_side_effects=True, vmem_limit_bytes=67043328
        ),
        name="attend",
    )(
        queries, keys, values, out_weight.T, query_gain[None], key_gain[None], out_gain[None],
        jnp.asarray(row_tab), jnp.asarray(col_tab), jnp.asarray(mats),
    )


def solution(mesh):
    return jax.shard_map(
        per_device,
        mesh=mesh,
        in_specs=(
            P("dp", "sp", None),
            P("dp", "sp", None),
            P("dp", "sp", None),
            P(),
            P(),
            P(None, "dp"),
            P(),
        ),
        out_specs=P("dp", "sp", None),
        check_vma=False,
    )
```

```python
import functools
import math

import jax
import jax.numpy as jnp
import numpy as np
from jax import lax
from jax.experimental import pallas as pl
from jax.experimental.pallas import tpu as pltpu
from jax.sharding import PartitionSpec as P

MESH = pl.DeviceIdType.MESH
F32 = jnp.float32
BF16 = jnp.bfloat16
NZ = 16
NX, NY = 4, 8
TOK = 192
LOG2E = math.log2(math.e)
EPS = 1e-06
MID = 10
SLOTS = 21
NC = 4
WTICKS = 20
N_RIGHT = (7, 7, 7, 7, 7, 7, 7, 7, 8, 8, 8, 8, 8, 8, 8, 7)
ORDER = (
    (
        (18895433, 6391506, 6391506, 543262416, 6391506, 6391506, 6391506, 799899, 537670683, 135083163, 135083163, 865435, 139277467, 135083163, 21836955, 5059739),
        (304521985, 692393044, 136348308, 201592850, 688133188, 688133260, 673227404, 17044628, 10818641, 446961672, 329586696, 489202433, 491127304, 329826824, 576884801, 692623368),
        (409045585, 153466578, 443369093, 409051466, 55412944, 55412760, 55588056, 56763945, 290326043, 293701146, 16877210, 17576146, 136414867, 136414874, 16790739, 86016657),
        (289743584, 690271965, 690267282, 172270872, 692328456, 692099080, 2490882, 36045443, 51675665, 51675793, 320118860, 413475468, 441357408, 329881610, 305439372, 220795649),
        (543262249, 136349403, 488937179, 443102538, 325714128, 444696216, 454046761, 543262377, 136423108, 36255939, 306561219, 25265690, 539002394, 201360922, 170037313, 413405250),
        (688198795, 323834976, 413438683, 463770266, 289711187, 159417408, 201597592, 692326593, 313268234, 73568321, 543330369, 543330385, 409588817, 285643858, 172401248, 21836956),
        (309200408, 335810755, 174702784, 460624475, 308917461, 443102378, 51217738, 409052440, 176195099, 201601242, 136393939, 21312723, 137363994, 293884424, 470569480, 407801921),
        (413406289, 51194449, 51675786, 176164875, 460231249, 155755162, 170439937, 692633672, 336351752, 403526273, 279713800, 327944769, 203456842, 21254794, 169911962, 136881820),
        (304481944, 289980611, 304719619, 51197258, 50451017, 424490218, 323827349, 23168666, 17118419, 17118880, 270927387, 136320211, 136911442, 319916609, 443646280, 443648520),
        (409045585, 543263297, 580944385, 289980483, 287941379, 158186057, 491066449, 447030017, 445221441, 313333761, 543263313, 35934304, 156242248, 176197827, 17109202, 136872602),
        (189081312, 2692314, 140608723, 50431657, 6391465, 470569032, 153957586, 304719514, 202122768, 17051803, 136348890, 173310721, 409741130, 57255145, 407750185, 309208616),
        (489428611, 324031105, 354985056, 692393164, 692396643, 21304979, 136427241, 443192401, 329818769, 458052684, 170218592, 844106305, 543228160, 409544704, 441264128, 488902736),
        (443136003, 16811731, 52965571, 327266328, 544047130, 326109000, 309663808, 690271442, 304428243, 172528730, 317402442, 988411635, 1073293211, 516554968, 373948440, 466560736),
        (869121178, 860705364, 458531916, 329585290, 866456657, 488969306, 488937115, 891590363, 508406353, 986393749, 443266238, 323856274, 307084442, 318584286, 528349086, 508116638),
        (937373691, 1046461850, 1073309598, 1073440499, 1073424094, 1073429747, 1073440499, 1073428379, 1073423763, 460318162, 460268691, 460924562, 508114138, 317564571, 306951898, 460177147),
        (937393655, 937393655, 937393655, 937393655, 937393655, 937393655, 937393655, 937393655, 937393655, 937393655, 937393655, 937393655, 937393655, 937393654, 937393654, 937393655),
    ),
    (
        (135561737, 341935808, 73500352, 411141824, 73500352, 73500352, 207718080, 543261912, 159483584, 17051803, 17051803, 23081115, 17138843, 21246107, 17044635, 135017627),
        (18129996, 312808529, 692453896, 136364096, 674238529, 411308097, 403997248, 137367616, 403998288, 56787468, 56795788, 404005516, 442671873, 325231361, 56764225, 145039968),
        (491569217, 153466011, 309143250, 323831301, 189890776, 288372229, 310478532, 56755752, 539002564, 136357572, 134529219, 170442947, 293634755, 674238529, 171016282, 18121226),
        (17052866, 690271965, 354751626, 707306123, 404005514, 51204746, 413406289, 292160009, 543951425, 453161056, 411840840, 588087624, 137113937, 51131547, 136938312, 135569932),
        (55332940, 151262939, 488937179, 174666970, 170442947, 170526235, 170505472, 170501845, 136877274, 688202336, 137367635, 201593368, 51684448, 220243020, 288690440, 437552204),
        (136386307, 325715485, 86020827, 457872458, 323857034, 6312586, 453154314, 51139082, 189806085, 424773144, 458241541, 17147432, 141312195, 711331904, 201621834, 169984195),
        (57770314, 413405249, 170922203, 409899595, 289739987, 289711828, 289740448, 170436308, 441754250, 84255370, 84218506, 409117324, 27531272, 201593347, 55413258, 56644234),
        (17080986, 21247650, 453783889, 159417027, 191440553, 443372627, 543273001, 202125640, 17044691, 323356187, 289800731, 170739224, 458494474, 17077418, 17044760, 169903828),
        (203726953, 411830849, 285553760, 140608746, 51687944, 86549130, 692393050, 86550161, 441819907, 174756945, 409056425, 19038858, 151262292, 425854661, 325666345, 458334536),
        (728340993, 189825235, 411141673, 86614785, 136648348, 23670995, 271099602, 293875907, 688132179, 413406298, 289740824, 325755649, 354762821, 355074568, 539001475, 176195200),
        (309212675, 57168392, 202146881, 201601235, 443560168, 447030024, 55877715, 458532490, 439355016, 407742488, 285775017, 335815176, 6398163, 409481347, 543262529, 153430609),
        (527034014, 21304516, 291602666, 51204616, 486842442, 192975040, 290039554, 170435226, 329816080, 337675330, 336344385, 376267945, 451782036, 466332820, 986426515, 978270109),
        (460928250, 459931979, 447025824, 692360916, 156014336, 158148426, 458135114, 174626005, 325793178, 995714217, 468429974, 451653338, 323727006, 306804383, 393033362, 309964499),
        (458041307, 392953526, 1070316787, 995833235, 987358933, 868858457, 913216081, 510601034, 986296023, 317402778, 307836567, 307177114, 307836115, 325662098, 323599507, 459125971),
        (936977559, 306783410, 306783706, 306951871, 317566651, 528039894, 528349086, 469628830, 392799378, 317535450, 392770771, 392799450, 466199762, 508404891, 392799450, 460269203),
        (937393655, 937393654, 937393654, 937393654, 937393654, 937393655, 937393655, 937393655, 937393654, 937393654, 937393654, 937393654, 937393655, 937393655, 937393654, 937393655),
    ),
)


def tables():
    freq = (10000.0 ** (-(np.arange(0, 32, 2, dtype=np.float32) / np.float32(32)))).astype(np.float32)
    lane = np.arange(256)
    is_row = lane % 64 < 32
    first = lane % 32 < 16
    sign = np.where(first, -1.0, 1.0)
    by_lane = freq[lane % 16]
    row_angle = (np.arange(48, dtype=np.float32)[:, None] * by_lane[None]).astype(np.float64)
    col_angle = (np.arange(64, dtype=np.float32)[:, None] * by_lane[None]).astype(np.float64)
    row_tab = np.zeros((NZ, 2, 8, 256), np.float32)
    row_tab[:, 0, :3] = np.where(is_row, np.cos(row_angle), 0).reshape(NZ, 3, 256)
    row_tab[:, 1, :3] = np.where(is_row, np.sin(row_angle) * sign, 0).reshape(NZ, 3, 256)
    col_tab = np.stack([np.where(is_row, 0, np.cos(col_angle)), np.where(is_row, 0, np.sin(col_angle) * sign)])
    partner = np.where(first, lane + 16, lane - 16)
    mats = np.zeros((2, 256, 256), np.float32)
    mats[0, partner, lane] = 1
    mats[1] = (lane[:, None] // 64 == lane[None] // 64) / 64.0
    return row_tab, col_tab.astype(np.float32), mats.astype(jnp.bfloat16)


def pick(values, z):
    out = jnp.int32(values[0])
    for i, v in enumerate(values[1:], 1):
        if v != values[0]:
            out = jnp.where(z == i, jnp.int32(v), out)
    return out


def gain_rows(gain):
    two = jnp.broadcast_to(jnp.concatenate([gain, gain], axis=1), (8, 128))
    lane = lax.broadcasted_iota(jnp.int32, (8, 128), 1)
    swapped = jnp.where(lane % 32 < 16, pltpu.roll(two, 112, 1), pltpu.roll(two, 16, 1))
    wide = lambda a: jnp.concatenate([a, a], axis=1)[0:1]
    return wide(two), wide(swapped)


def rope(x, gain, row_tab, col_tab, mats):
    g, gp = gain
    xf = x.astype(F32)
    sq = xf * xf
    hi = sq.astype(BF16)
    lo = (sq - hi.astype(F32)).astype(BF16)
    mean = jnp.dot(hi, mats[1], preferred_element_type=F32) + jnp.dot(lo, mats[1], preferred_element_type=F32)
    xp = jnp.dot(x, mats[0], preferred_element_type=F32)
    r = lax.rsqrt(mean + EPS)
    parts = []
    for i in range(3):
        rows = slice(64 * i, 64 * i + 64)
        c = (col_tab[0] + row_tab[0, i : i + 1, :]) * g
        s = (col_tab[1] + row_tab[1, i : i + 1, :]) * gp
        parts.append((xf[rows] * c + xp[rows] * s) * r[rows])
    return jnp.concatenate(parts, axis=0)


def kernel(
    q_hbm, k_hbm, v_hbm, w_hbm, qg_hbm, kg_hbm, og_hbm, row_hbm, col_hbm, mats_hbm,
    out_ref,
    qb, kraw, row_tab, col_tab, mats, qg_ref, kg_ref, og_ref,
    KV, VT, WB, QX, KX, M, L, MB, E, OT, ATT, PROJ,
    in_sem, s_sem, r_sem, wx_ss, wx_rs, wy_ss, wy_rs, wd_ss, wd_rs, late_sem,
):
    z = lax.axis_index("sp")
    d = lax.axis_index("dp")
    core = d & 1
    x = (d >> 1) & (NX - 1)
    y = d >> 3
    up, down = (z + 1) & (NZ - 1), (z - 1) & (NZ - 1)
    at = lambda xx, yy, cc: (z, (yy * NX + xx) * 2 + cc)
    nR = pick(N_RIGHT, z)
    nL = (NZ - 1) - nR
    low = MID - nR

    loads = [
        pltpu.make_async_copy(k_hbm.at[0], kraw, in_sem.at[0]),
        pltpu.make_async_copy(row_hbm.at[z], row_tab, in_sem.at[1]),
        pltpu.make_async_copy(col_hbm, col_tab, in_sem.at[2]),
        pltpu.make_async_copy(mats_hbm, mats, in_sem.at[3]),
        pltpu.make_async_copy(kg_hbm, kg_ref, in_sem.at[7]),
        pltpu.make_async_copy(v_hbm.at[0], KV.at[MID + SLOTS], in_sem.at[4]),
        pltpu.make_async_copy(w_hbm, WB.at[d], in_sem.at[5]),
        pltpu.make_async_copy(q_hbm.at[0], qb, in_sem.at[6]),
        pltpu.make_async_copy(qg_hbm, qg_ref, in_sem.at[8]),
        pltpu.make_async_copy(og_hbm, og_ref, in_sem.at[9]),
    ]
    for c in loads:
        c.start()

    barrier = pltpu.get_barrier_semaphore()
    sib = at(x, y, 1 - core)
    partners = [
        (down, d),
        at((x + 1) & (NX - 1), y, core), at((x + 2) & (NX - 1), y, core), at((x + 3) & (NX - 1), y, core),
        at(x, (y + 1) & (NY - 1), core), at(x, (y - 1) & (NY - 1), core), sib,
    ]
    for p in partners:
        pl.semaphore_signal(barrier, inc=1, device_id=p, device_id_type=MESH)

    @pl.when(z != NZ - 1)
    def _():
        pl.semaphore_signal(barrier, inc=1, device_id=(up, d), device_id_type=MESH)

    for c in loads[:5]:
        c.wait()
    kg = gain_rows(kg_ref[...])
    KV[MID] = rope(kraw[...], kg, row_tab, col_tab, mats).astype(BF16)
    loads[5].wait()
    loads[6].wait()
    pl.semaphore_wait(barrier, len(partners) + jnp.where(z == 0, 0, 1))

    @pl.when(z == NZ - 1)
    def _():
        pl.semaphore_signal(late_sem, inc=1, device_id=(0, d), device_id_type=MESH)

    there = lambda sg: jnp.where(sg < 0, up, down)

    def kv(b, sg, c):
        rows = pl.ds(c * (TOK // NC), TOK // NC)
        return pltpu.make_async_remote_copy(
            src_ref=KV.at[b, rows], dst_ref=KV.at[b + sg, rows], send_sem=s_sem.at[(sg + 1) >> 1],
            recv_sem=r_sem.at[b + sg, c], device_id=(there(sg), d), device_id_type=MESH,
        )

    def own(b, sg):
        for c in range(NC):
            kv(b, sg, c).start()

    own(MID, -1)

    @pl.when(z == 0)
    def _():
        own(MID + SLOTS, -1)

    @pl.when(z != 0)
    def _():
        own(MID, 1)

    def wx(j):
        return pltpu.make_async_remote_copy(
            src_ref=WB.at[d], dst_ref=WB.at[d], send_sem=wx_ss, recv_sem=wx_rs.at[j],
            device_id=at((x - j) & (NX - 1), y, core), device_id_type=MESH,
        )

    def wblock(j, s):
        return (((y - s) & (NY - 1)) * NX + ((x + j) & (NX - 1))) * 2 + core

    def wy(j, s, sg):
        blk = wblock(j, -sg * s)
        return pltpu.make_async_remote_copy(
            src_ref=WB.at[blk], dst_ref=WB.at[blk], send_sem=wy_ss,
            recv_sem=wy_rs.at[(sg + 1) >> 1, j, s + 1],
            device_id=at(x, (y - sg) & (NY - 1), core), device_id_type=MESH,
        )

    def wd(blk):
        return pltpu.make_async_remote_copy(
            src_ref=WB.at[blk], dst_ref=WB.at[blk], send_sem=wd_ss, recv_sem=wd_rs,
            device_id=sib, device_id_type=MESH,
        )

    for j in (1, 2, 3):
        wx(j).start()
    wd(d).start()

    def w_side(j, s, sg, upto):
        most = upto(j, sg)
        blk = wblock(j, -sg * s)

        @pl.when(s <= most)
        def _():
            wy(j, s - 1, sg).wait_recv()
            wd(blk).start()

        @pl.when(s + 1 <= most)
        def _():
            wy(j, s, sg).start()

    def upto(j, sg):
        even = 1 - (j & 1)
        return jnp.where(sg < 0, 3 + even, 4 - even)

    def w_tick(i):
        s, j = i >> 2, i & 3

        @pl.when(s == 0)
        def _():
            @pl.when(j > 0)
            def _():
                wx(j).wait_recv()
                wd(wblock(j, 0)).start()

            wy(j, s, -1).start()
            wy(j, s, 1).start()

        @pl.when(s > 0)
        def _():
            w_side(j, s, -1, upto)
            w_side(j, s, 1, upto)

    for c in loads[7:]:
        c.wait()
    qg = gain_rows(qg_ref[...])
    lane = lax.broadcasted_iota(jnp.int32, (64, 128), 1)

    def put(t, half, val):
        hi = val.astype(BF16)
        rest = val - hi.astype(F32)
        mid = rest.astype(BF16)
        lo = (rest - mid.astype(F32)).astype(BF16)
        cols = slice(128 * half, 128 * half + 128)
        QX[t, 0:64, cols] = hi
        QX[t, 64:128, cols] = mid
        QX[t, 128:192, cols] = lo
        QX[t, 192:256, cols] = jnp.zeros((64, 128), BF16)

    for g in range(4):
        qr = rope(qb[:, 256 * g : 256 * g + 256], qg, row_tab, col_tab, mats)
        qr = qr.astype(BF16).astype(F32) * (0.125 * LOG2E)
        a = jnp.transpose(qr[0:128])
        b = jnp.transpose(jnp.concatenate([qr[128:192], jnp.zeros((64, 256), F32)], axis=0))
        for r in range(4):
            put(3 * g + r // 2, r % 2, a[64 * r : 64 * r + 64])
        for h in range(2):
            b0, b1 = b[128 * h : 128 * h + 64], pltpu.roll(b[128 * h + 64 : 128 * h + 128], 64, 1)
            put(3 * g + 2, h, jnp.where(lane < 64, b0, b1))
    M[...] = jnp.full_like(M, -1e30)
    L[...] = jnp.zeros_like(L)
    OT[...] = jnp.zeros_like(OT)
    lane2 = lax.broadcasted_iota(jnp.int32, (TOK, 128), 1)

    def pass1(b):
        for pr in range(2):
            v = KV[b, :, 128 * pr : 128 * pr + 128].astype(F32)
            rt = pltpu.roll(v, 64, 1)
            for o in range(2):
                dup = jnp.where(lane2 < 64, v, rt) if o == 0 else jnp.where(lane2 < 64, rt, v)
                dup = dup.astype(BF16)
                KX[2 * pr + o, :, 0:128] = dup
                KX[2 * pr + o, :, 128:256] = dup
        i = b - low
        for t in range(12):
            s = jnp.dot(KX[t // 3], QX[t], preferred_element_type=F32).reshape(TOK // 8, 8, 256)
            old = M[t]
            new = jnp.maximum(old, jnp.max(s, axis=0))
            e = jnp.exp2(s - new[None])
            L[t] = L[t] * jnp.exp2(old - new) + jnp.sum(e, axis=0)
            M[t] = new
            MB[i, t] = new
            E[i, t] = e.reshape(TOK, 256)

    def pass2(m):
        v = KV[pl.ds(SLOTS + low + 2 * m, 2)].reshape(2 * TOK, 256)
        for c in range(3):
            VT[:, 128 * c : 128 * c + 128] = jnp.transpose(v[128 * c : 128 * c + 128].astype(F32)).astype(BF16)
        for t in range(12):
            g = t // 3
            p = []
            for i in (2 * m, 2 * m + 1):
                f = jnp.exp2(MB[i, t] - M[t])
                p.append((E[i, t].reshape(TOK // 8, 8, 256) * f[None]).reshape(TOK, 256).astype(BF16))
            OT[t] += jnp.dot(VT[64 * g : 64 * g + 64], jnp.concatenate(p, axis=0), preferred_element_type=F32)

    pass1(MID)

    @pl.when(z == 0)
    def _():
        pl.semaphore_wait(late_sem, 1)
        own(MID, 1)

    def finish():
        m = M[...]
        top = jnp.max(m, axis=1, keepdims=True)
        total = jnp.sum(L[...] * jnp.exp2(m - top), axis=1, keepdims=True)
        M[...] = jnp.broadcast_to(top + jnp.log(total) * LOG2E, M.shape)

    shift = NC.bit_length() - 1
    right_up, left_down = pick(N_RIGHT[1:] + N_RIGHT[:1], z), (NZ - 1) - pick(N_RIGHT[-1:] + N_RIGHT[:-1], z)

    def step(_, carry):
        word, copies, blocks, done = carry
        digit = word & 7
        side = digit & 1
        sg = 2 * side - 1
        is_copy = digit < 4
        c_at, b_at = 6 * (digit & 3), 4 * (digit & 3)

        @pl.when(is_copy)
        def _():
            n = (copies >> c_at) & 63
            v = digit >> 1
            k = (n >> shift) + 1 - v
            c = n & (NC - 1)
            b = MID + sg * k + SLOTS * v

            @pl.when(k > 0)
            def _():
                kv(b - sg, sg, c).wait_recv()

            @pl.when(k < jnp.where(side == 0, right_up, left_down))
            def _():
                kv(b, sg, c).start()

        n = (blocks >> b_at) & 15
        b = MID + sg * (n + 1)
        is_scores = (digit == 4) | (digit == 5)

        @pl.when(is_scores)
        def _():
            pass1(b)

            def w(j, c):
                w_tick(j)
                return c

            lax.fori_loop((3 * done) >> 1, jnp.minimum((3 * done + 3) >> 1, WTICKS), w, 0)

            @pl.when(done == NZ - 2)
            def _():
                finish()

        @pl.when((digit >= 6) & (n < 4))
        def _():
            pass2(jnp.where(side == 0, 3 - n, 4 + n))

        one = jnp.int32(1)
        return (
            word >> 3,
            copies + jnp.where(is_copy, one << c_at, 0),
            blocks + jnp.where(is_copy, 0, one << b_at),
            done + jnp.where(is_scores, 1, 0),
        )

    def ten(_, carry):
        words, counts = carry
        out = lax.fori_loop(0, 10, step, (words[0], *counts))
        return words[1:] + words[:1], out[1:]

    zero = jnp.int32(0)
    counts = (jnp.where(z == 0, jnp.int32(NC << 12), 0), zero, zero)
    words = tuple(jnp.where(core == 0, pick(a, z), pick(b, z)) for a, b in zip(*ORDER))
    lax.fori_loop(0, len(words), ten, (words, counts))

    for g in range(4):
        for p in range(2):
            a = jnp.concatenate([OT[3 * g + p, :, 0:128], OT[3 * g + p, :, 128:256]], axis=0)
            ATT[0:128, 256 * g + 128 * p : 256 * g + 128 * p + 128] = jnp.transpose(a).astype(BF16)
            b = OT[3 * g + 2, :, 128 * p : 128 * p + 128]
            b = jnp.transpose(jnp.concatenate([b, b], axis=0))
            ATT[128:192, 256 * g + 128 * p : 256 * g + 128 * p + 128] = jnp.where(lane < 64, b[0:64], b[64:128]).astype(BF16)

    def all_w(n, ss, rs):
        part = WB.at[pl.ds(0, n)]
        return pltpu.make_async_remote_copy(
            src_ref=part, dst_ref=part, send_sem=ss, recv_sem=rs, device_id=sib, device_id_type=MESH
        )

    all_w(NX * NY, wd_ss, wd_rs).wait_recv()

    w = WB[...].reshape(2048, 1024)
    pr = lax.dot_general(ATT[...], w, (((1,), (1,)), ((), ())), preferred_element_type=F32)
    PROJ[...] = pr
    sq = pr * pr
    ss = sum(sq[:, 128 * c : 128 * c + 128] for c in range(16))
    r = lax.rsqrt(jnp.sum(ss, axis=1, keepdims=True) / 2048.0 + EPS)
    for i in range(3):
        rows = slice(64 * i, 64 * i + 64)
        out_ref[0, rows] = (PROJ[rows] * r[rows] * og_ref[...]).astype(BF16)

    for side, n, values in ((0, right_up, set(N_RIGHT)), (1, left_down, {NZ - 1 - v for v in N_RIGHT})):
        for v in sorted(values):

            @pl.when(n == v)
            def _():
                part = KV.at[pl.ds(0, 2 * v)]
                pltpu.make_async_remote_copy(
                    src_ref=part, dst_ref=part, send_sem=s_sem.at[side], recv_sem=s_sem.at[side],
                    device_id=(up, d), device_id_type=MESH,
                ).wait_send()

    all_w(3, wx_ss, wd_rs).wait_send()
    all_w(28, wy_ss, wd_rs).wait_send()
    all_w(NX * NY, wd_ss, wd_rs).wait_send()


def per_device(queries, keys, values, query_gain, key_gain, out_weight, out_gain):
    row_tab, col_tab, mats = tables()
    hbm = pl.BlockSpec(memory_space=pl.ANY)
    dma = pltpu.SemaphoreType.DMA
    return pl.pallas_call(
        kernel,
        out_shape=pltpu.VMEM((1, TOK, 2048), BF16),
        in_specs=[hbm] * 10,
        out_specs=pl.BlockSpec(memory_space=pltpu.VMEM),
        scratch_shapes=[
            pltpu.VMEM((TOK, 1024), BF16), pltpu.VMEM((TOK, 256), BF16),
            pltpu.VMEM((2, 8, 256), F32), pltpu.VMEM((2, 64, 256), F32), pltpu.VMEM((2, 256, 256), BF16),
            pltpu.VMEM((1, 64), F32), pltpu.VMEM((1, 64), F32), pltpu.VMEM((1, 2048), F32),
            pltpu.VMEM((2 * SLOTS, TOK, 256), BF16), pltpu.VMEM((256, 2 * TOK), BF16),
            pltpu.VMEM((64, 32, 1024), BF16), pltpu.VMEM((12, 256, 256), BF16), pltpu.VMEM((4, TOK, 256), BF16),
            pltpu.VMEM((12, 8, 256), F32), pltpu.VMEM((12, 8, 256), F32), pltpu.VMEM((NZ, 12, 8, 256), F32),
            pltpu.VMEM((NZ, 12, TOK, 256), F32), pltpu.VMEM((12, 64, 256), F32), pltpu.VMEM((TOK, 1024), BF16),
            pltpu.VMEM((TOK, 2048), F32),
            dma((10,)), dma((2,)), dma((2 * SLOTS, NC)),
            dma, dma((4,)), dma, dma((2, 4, 5)), dma, dma, pltpu.SemaphoreType.REGULAR,
        ],
        compiler_params=pltpu.CompilerParams(
            collective_id=0, has_side_effects=True, vmem_limit_bytes=58000000
        ),
        name="attend",
    )(
        queries, keys, values, out_weight.T, query_gain[None], key_gain[None], out_gain[None],
        jnp.asarray(row_tab), jnp.asarray(col_tab), jnp.asarray(mats),
    )


def solution(mesh):
    return jax.shard_map(
        per_device,
        mesh=mesh,
        in_specs=(
            P("dp", "sp", None),
            P("dp", "sp", None),
            P("dp", "sp", None),
            P(),
            P(),
            P(None, "dp"),
            P(),
        ),
        out_specs=P("dp", "sp", None),
        check_vma=False,
    )
```
